32 devices in a mesh: ep: 8 (over z, x), tp: 4 (over y, core).
Axes of the slice: x: 2, y: 2, z: 4, core: 2. Of those that a mesh axis runs over, the one named last changes fastest.
Arguments:
- mixer_input: bfloat16 [5120, 2048], P('ep'), may hold values from -6 to 6
- mixer_gain: float32 [2048], replicated, may hold values from 0.1 to 1.9
- value_weight: bfloat16 [2048, 1024], P(None, 'tp'), may hold values from -0.125 to 0.125
- inner_gate: bfloat16 [2048, 1024], P(None, 'tp'), may hold values from -0.125 to 0.125
- outer_gate: bfloat16 [2048, 1024], P(None, 'tp'), may hold values from -0.125 to 0.125
- kernel_taps: float32 [3, 1024], P(None, 'tp'), may hold values from -3 to 3
- mixer_proj: bfloat16 [1024, 2048], P('tp'), may hold values from -0.1875 to 0.1875
- expert_input: bfloat16 [5120, 2048], P(('ep', 'tp')), may hold values from -6 to 6
- expert_gain: float32 [2048], replicated, may hold values from 0.1 to 1.9
- routes: int32 [5120, 2], P(('ep', 'tp')), may hold values from 0 to 7, as said below
- group_logits: float32 [5120, 1], P(('ep', 'tp')), may hold values from -6 to 6
- pair_logits: float32 [5120, 2], P(('ep', 'tp')), may hold values from -6 to 6
- gate_weight: bfloat16 [8, 2048, 1024], P('ep', None, 'tp'), may hold values from -0.125 to 0.125
- up_weight: bfloat16 [8, 2048, 1024], P('ep', None, 'tp'), may hold values from -0.125 to 0.125
- down_weight: bfloat16 [8, 1024, 2048], P('ep', 'tp'), may hold values from -0.75 to 0.75
Outputs:
- mixer_output: bfloat16 [5120, 2048], P(('ep', 'tp'))
- expert_output: bfloat16 [5120, 2048], P(('ep', 'tp'))
The draws below stay inside these ranges and needn't reach their ends.
Inputs may be any that keep to these rules, and one draw needn't show every extreme that they name: `routes`: both entries of a row are different experts of one group (equal after integer division by 8). In the rows of one device every group is chosen by the same number of rows, no expert is named more than 80 times, and in every draw one expert is named exactly 80 times in the rows of every device.
All inputs are finite; a program needn't handle non-finite values.
Results may differ from the reference program's by a relative error of at most 0.01.
Values may be sent and summed in bfloat16 or wider, within the bound.
A program may use at most 128 MiB of HBM per device.

```python
import jax
import jax.numpy as jnp
from jax import lax

D = 2048
CW = 1024
TAPS = 3
FF = 1024
EPG = 8
TOK_DEV = 160
GROUPS = 1
EXPERTS = 8
CAP = 80
TOKENS = 5120
N_EP = 8
N_TP = 4


def route_block(key, heavy, light):
    share = CAP // 2
    keys = jax.random.split(key, 4)
    group = jax.random.randint(keys[0], (), 0, GROUPS)
    order = jax.random.permutation(keys[1], EPG)
    raised = group * EPG + order[0]
    lowered = group * EPG + order[1]
    if share >= 2:
        shift = jax.random.randint(keys[2], (), 1, share)
    else:
        shift = jnp.zeros((), jnp.int32)
    clear = (raised != heavy) & (raised != light) & (lowered != heavy) & (lowered != light)
    shift = jnp.where(clear, shift, 0)
    experts_iota = jnp.arange(EXPERTS, dtype=jnp.int32)
    loads = (share + share * (experts_iota == heavy) - share * (experts_iota == light) + shift * (experts_iota == raised) - shift * (experts_iota == lowered)).astype(jnp.int32)
    bounds = jnp.cumsum(loads)
    per_group = EPG * share // 2
    place = jnp.arange(TOK_DEV, dtype=jnp.int32)
    first_slot = place // per_group * (2 * per_group) + place % per_group
    second_slot = first_slot + per_group
    first = jnp.sum((bounds[None, :] <= first_slot[:, None]).astype(jnp.int32), axis=1)
    second = jnp.sum((bounds[None, :] <= second_slot[:, None]).astype(jnp.int32), axis=1)
    pairs = jnp.stack([first, second], axis=1).astype(jnp.int32)
    shuffle = jax.random.permutation(keys[3], TOK_DEV)
    return jnp.zeros((TOK_DEV, 2), jnp.int32).at[shuffle].set(pairs)


def draw_routes(key, part):
    base = jax.random.fold_in(key, 17)
    picks = jax.random.split(jax.random.fold_in(base, 1), 2)
    group = jax.random.randint(picks[0], (), 0, GROUPS)
    order = jax.random.permutation(picks[1], EPG)
    heavy = group * EPG + order[0]
    light = group * EPG + order[1]
    block_keys = jax.random.split(jax.random.fold_in(base, 2), TOKENS // TOK_DEV)

    def one_block(block_key):
        return route_block(block_key, heavy, light)
    routed = jax.vmap(one_block)(block_keys)
    return routed.reshape(TOKENS, 2)


def level_of(key, dims, shards, smallest, largest):
    level = 1.0
    for position, shards_of in shards:
        steps = jax.random.uniform(jax.random.fold_in(jax.random.fold_in(key, 6), position), (shards_of,), jnp.float32, smallest / len(shards), largest / len(shards))
        level = level * jnp.repeat(jnp.exp(steps), dims[position] // shards_of).reshape((-1,) + (1,) * (len(dims) - 1 - position))
    return level


def normal_values(rng, extent, deviation, bound, cuts=(), kind=jnp.bfloat16):
    level = level_of(rng, extent, cuts, -0.22, 0.18) if cuts else 1.0
    drawn = jax.random.normal(rng, extent, jnp.float32) * deviation * level
    return jnp.minimum(jnp.maximum(drawn, -bound), bound).astype(kind)


def setup_inputs(seed: int = 0) -> dict:
    key_list = jax.random.split(jax.random.key(seed), 16)
    return {
        "mixer_input": normal_values(key_list[0], (TOKENS, D), 1.0, 6.0, ((0, 8),)),
        "mixer_gain": jnp.clip(1.0 + 0.18 * jax.random.normal(key_list[1], (D,), jnp.float32), 0.1, 1.9),
        "value_weight": normal_values(key_list[2], (D, CW), D ** -0.5, 0.125, ((1, 4),)),
        "inner_gate": normal_values(key_list[3], (D, CW), D ** -0.5, 0.125, ((1, 4),)),
        "outer_gate": normal_values(key_list[4], (D, CW), D ** -0.5, 0.125, ((1, 4),)),
        "kernel_taps": normal_values(key_list[5], (TAPS, CW), 0.6, 3.0, ((1, 4),), jnp.float32),
        "mixer_proj": normal_values(key_list[6], (CW, D), CW ** -0.5, 0.1875, ((0, 4),)),
        "expert_input": normal_values(key_list[7], (TOKENS, D), 1.0, 6.0, ((0, 32),)),
        "expert_gain": jnp.clip(1.0 + 0.18 * jax.random.normal(key_list[8], (D,), jnp.float32), 0.1, 1.9),
        "routes": draw_routes(jax.random.fold_in(key_list[15], 71), 0),
        "group_logits": normal_values(key_list[10], (TOKENS, GROUPS), 1.5, 6.0, ((0, 32),), jnp.float32),
        "pair_logits": normal_values(key_list[11], (TOKENS, 2), 1.5, 6.0, ((0, 32),), jnp.float32),
        "gate_weight": normal_values(key_list[12], (EXPERTS, D, FF), D ** -0.5, 0.125, ((0, 8), (2, 4))),
        "up_weight": normal_values(key_list[13], (EXPERTS, D, FF), D ** -0.5, 0.125, ((0, 8), (2, 4))),
        "down_weight": normal_values(key_list[14], (EXPERTS, FF, D), (FF // 16) ** -0.5, 0.75, ((0, 8), (1, 4))),
    }


EPSILON = 1e-06

def normed(values, gain):
    wide = values.astype(jnp.float32)
    scale = lax.rsqrt(lax.optimization_barrier(jnp.mean(wide * wide, axis=-1, keepdims=True)) + EPSILON)
    return (wide * scale * gain).astype(jnp.bfloat16)

def blockwise_sum(left, right, blocks):
    width = left.shape[1] // blocks
    total = jnp.zeros((left.shape[0], right.shape[1]), jnp.float32)
    for block in range(blocks):
        part = jnp.dot(left[:, block * width:(block + 1) * width], right[block * width:(block + 1) * width], preferred_element_type=jnp.float32)
        rounded = lax.optimization_barrier(part.astype(jnp.bfloat16))
        total = total + rounded.astype(jnp.float32)
    return total.astype(jnp.bfloat16)

def route_weights(routes, group_logits, pair_logits):
    chosen = routes[:, 0] // EPG
    groups = jnp.arange(group_logits.shape[1], dtype=jnp.int32)
    picked = lax.optimization_barrier(jnp.sum(jnp.where(groups[None, :] == chosen[:, None], group_logits, 0.0), axis=1))
    group_weight = 1.0 / lax.optimization_barrier(jnp.sum(jnp.exp(group_logits - picked[:, None]), axis=1))
    return group_weight[:, None] * jax.nn.sigmoid(pair_logits - pair_logits[:, ::-1])

def expert_block(rows, gate, upper, down, blocks):
    first = jnp.dot(rows, gate, preferred_element_type=jnp.float32)
    second = jnp.dot(rows, upper, preferred_element_type=jnp.float32)
    hidden = (jax.nn.silu(first) * second).astype(jnp.bfloat16)
    return blockwise_sum(hidden, down, blocks)

def reference(mixer_input, mixer_gain, value_weight, inner_gate, outer_gate, kernel_taps, mixer_proj, expert_input, expert_gain, routes, group_logits, pair_logits, gate_weight, up_weight, down_weight):
    normal_rows = normed(mixer_input, mixer_gain)
    values = jnp.dot(normal_rows, value_weight, preferred_element_type=jnp.float32)
    inner = jnp.dot(normal_rows, inner_gate, preferred_element_type=jnp.float32)
    outer = jnp.dot(normal_rows, outer_gate, preferred_element_type=jnp.float32)
    mixed_in = (inner * values).astype(jnp.bfloat16)
    padded = jnp.pad(mixed_in, ((1, 1), (0, 0))).astype(jnp.float32)
    conv_sum = kernel_taps[0] * padded[:-2] + kernel_taps[1] * padded[1:-1] + kernel_taps[2] * padded[2:]
    mixer_rows = (outer * conv_sum).astype(jnp.bfloat16)
    mixer_output = blockwise_sum(mixer_rows, mixer_proj, N_TP)
    expert_norm = normed(expert_input, expert_gain)
    weights = route_weights(routes, group_logits, pair_logits)
    flat = routes.reshape(-1)
    count = flat.shape[0]
    order = jnp.argsort(flat, stable=True).astype(jnp.int32)
    experts_iota = jnp.arange(EXPERTS, dtype=jnp.int32)
    loads = lax.optimization_barrier(jnp.sum((flat[:, None] == experts_iota[None, :]).astype(jnp.int32), axis=0))
    starts = (jnp.cumsum(loads) - loads).astype(jnp.int32)
    most = N_EP * N_TP * CAP
    padded_order = jnp.concatenate([order, jnp.full((most,), count, jnp.int32)])
    rows_pad = jnp.concatenate([expert_norm, jnp.zeros((1, D), jnp.bfloat16)])

    def one_expert(results, expert):
        picks = lax.dynamic_slice_in_dim(padded_order, starts[expert], most)
        live = jnp.arange(most, dtype=jnp.int32) < loads[expert]
        picks = jnp.where(live, picks, count).astype(jnp.int32)
        sources = jnp.where(live, picks // 2, count // 2).astype(jnp.int32)
        answers = expert_block(rows_pad[sources], gate_weight[expert], up_weight[expert], down_weight[expert], N_TP)
        return (results.at[picks].set(answers), None)
    results = jnp.zeros((count + 1, D), jnp.bfloat16)
    results, _ = lax.scan(one_expert, results, experts_iota)
    pairs = results[:count].reshape(count // 2, 2, D).astype(jnp.float32)
    expert_output = lax.optimization_barrier(jnp.sum(weights[:, :, None] * pairs, axis=1)).astype(jnp.bfloat16)
    return (mixer_output, expert_output)
```

```python
import functools

import jax
import jax.numpy as jnp
from jax import lax
from jax.experimental import pallas as pl
from jax.experimental.pallas import tpu as pltpu
from jax.sharding import PartitionSpec as P

EPG = 8


EPSILON = 1e-06


def padded_2(cells, sides, width):
    for axis, dim in sides:
        count = lax.axis_size(axis)
        ends = count - 1
        head = lax.slice_in_dim(cells, 0, width, axis=dim)
        tail = lax.slice_in_dim(cells, cells.shape[dim] - width, cells.shape[dim], axis=dim)
        cells = jnp.concatenate(
            [
                lax.ppermute(tail, axis, [(i, (i + 1) % count) for i in range(ends)]),
                cells,
                lax.ppermute(head, axis, [((i + 1) % count, i) for i in range(ends)]),
            ],
            axis=dim,
        )
    return cells


def normed(values, gain):
    wide = values.astype(jnp.float32)
    scale = lax.rsqrt(jnp.mean(wide * wide, axis=-1, keepdims=True) + EPSILON)
    return (wide * scale * gain).astype(jnp.bfloat16)


def route_weights(routes, group_logits, pair_logits):
    chosen = routes[:, 0] // EPG
    groups = jnp.arange(group_logits.shape[1], dtype=jnp.int32)
    picked = jnp.sum(jnp.where(groups[None, :] == chosen[:, None], group_logits, 0.0), axis=1)
    group_weight = 1.0 / jnp.sum(jnp.exp(group_logits - picked[:, None]), axis=1)
    return group_weight[:, None] * jax.nn.sigmoid(pair_logits - pair_logits[:, ::-1])


def on_device(
    mixer_input,
    mixer_gain,
    value_weight,
    inner_gate,
    outer_gate,
    kernel_taps,
    mixer_proj,
    expert_input,
    expert_gain,
    routes,
    group_logits,
    pair_logits,
    gate_weight,
    up_weight,
    down_weight,
):
    normal_rows = normed(mixer_input, mixer_gain)
    values = jnp.dot(normal_rows, value_weight, preferred_element_type=jnp.float32)
    inner = jnp.dot(normal_rows, inner_gate, preferred_element_type=jnp.float32)
    outer = jnp.dot(normal_rows, outer_gate, preferred_element_type=jnp.float32)
    mixed_in = (inner * values).astype(jnp.bfloat16)
    padded = padded_2(mixed_in, (("ep", 0),), 1).astype(jnp.float32)
    conv_sum = (
        kernel_taps[0] * padded[:-2] + kernel_taps[1] * padded[1:-1] + kernel_taps[2] * padded[2:]
    )
    mixer_rows = (outer * conv_sum).astype(jnp.bfloat16)
    mixer_output = lax.psum_scatter(
        jnp.dot(mixer_rows, mixer_proj, preferred_element_type=jnp.float32).astype(jnp.bfloat16),
        "tp",
        scatter_dimension=0,
        tiled=True,
    )
    weights = route_weights(routes, group_logits, pair_logits)
    experts = lax.axis_size("ep")
    local, width = expert_input.shape
    capacity = 4 * local // experts
    picks = slot_masks(routes, experts, capacity)
    outgoing = dispatch(expert_input, expert_gain, routes, experts, capacity)
    arrived = lax.all_to_all(
        outgoing.reshape(experts, capacity, width), "ep", split_axis=0, concat_axis=0, tiled=True
    ).reshape(experts * capacity, width)
    gates = tp_pieces(gate_weight[0], mixer_rows)
    ups = tp_pieces(up_weight[0], mixer_rows)
    downs = tp_pieces(down_weight[0], mixer_rows)
    answers = expert_block_local(arrived, gates, ups, downs)
    answered = lax.all_to_all(
        answers.reshape(experts, capacity, width), "ep", split_axis=0, concat_axis=0, tiled=True
    ).reshape(experts * capacity, width)
    mix = jnp.where(picks[0], weights[:, 0:1], 0.0) + jnp.where(picks[1], weights[:, 1:2], 0.0)
    coarse = lax.reduce_precision(mix, 8, 7)
    fine = (mix - coarse).astype(jnp.bfloat16)
    expert_output = (
        jnp.dot(coarse.astype(jnp.bfloat16), answered, preferred_element_type=jnp.float32)
        + jnp.dot(fine, answered, preferred_element_type=jnp.float32)
    ).astype(jnp.bfloat16)
    return (mixer_output, expert_output)


def dispatch_kernel(experts, capacity, values_ref, gain_ref, routes_ref, out_ref):
    local = values_ref.shape[0]
    normal_rows = normed(values_ref[...], gain_ref[...])
    names = lax.broadcasted_iota(jnp.int32, (experts, local), 0)
    bases = (names * capacity).astype(jnp.float32)
    earlier = lax.broadcasted_iota(jnp.int32, (local, local), 0)
    later = lax.broadcasted_iota(jnp.int32, (local, local), 1)
    before = jnp.where(earlier < later, 1.0, 0.0).astype(jnp.bfloat16)
    rows = lax.broadcasted_iota(jnp.int32, (experts * capacity, local), 0)
    chosen = None
    taken = jnp.zeros((experts, 1), jnp.float32)
    for k in range(2):
        named = names == routes_ref[k : k + 1, :]
        ones = jnp.where(named, 1.0, 0.0)
        rank = jnp.dot(ones.astype(jnp.bfloat16), before, preferred_element_type=jnp.float32)
        slot = jnp.sum(ones * (rank + bases + taken), axis=0, keepdims=True).astype(jnp.int32)
        taken = taken + jnp.sum(ones, axis=1, keepdims=True)
        mask = jnp.where(rows == slot, 1.0, 0.0)
        chosen = mask if chosen is None else chosen + mask
    out_ref[...] = jnp.dot(
        chosen.astype(jnp.bfloat16), normal_rows, preferred_element_type=jnp.float32
    ).astype(jnp.bfloat16)


def dispatch(values, gain, routes, experts, capacity):
    local, width = values.shape
    return pl.pallas_call(
        functools.partial(dispatch_kernel, experts, capacity),
        out_shape=jax.ShapeDtypeStruct((experts * capacity, width), jnp.bfloat16),
        cost_estimate=pl.CostEstimate(
            flops=2 * experts * capacity * local * width,
            bytes_accessed=2 * (local + experts * capacity) * width,
            transcendentals=0,
        ),
    )(values, gain.reshape(1, width), routes.T)


def slot_masks(routes, experts, capacity):
    local = routes.shape[0]
    place = jnp.arange(local, dtype=jnp.int32)
    earlier = (place[None, :] < place[:, None]).astype(jnp.bfloat16)
    names = jnp.arange(experts, dtype=jnp.int32)
    named = [routes[:, k : k + 1] == names[None, :] for k in range(2)]
    ranks = [
        jnp.dot(earlier, one.astype(jnp.bfloat16), preferred_element_type=jnp.float32)
        for one in named
    ]
    ranks[1] = ranks[1] + jnp.sum(named[0].astype(jnp.float32), axis=0, keepdims=True)
    rows = jnp.arange(experts * capacity, dtype=jnp.int32)
    bases = (names * capacity).astype(jnp.float32)
    masks = []
    for one, rank in zip(named, ranks):
        slot = jnp.sum(jnp.where(one, rank + bases, 0.0), axis=1, keepdims=True).astype(jnp.int32)
        masks.append(slot == rows[None, :])
    return masks


def tp_pieces(piece, after):
    count = lax.axis_size("tp")
    pieces = [piece]
    step = count // 2
    while step:
        pairs = [(i, i ^ step) for i in range(count)]
        if len(pieces) == 2:
            pieces[1], _ = lax.optimization_barrier((pieces[1], after))
        pieces = pieces + [lax.ppermute(held, "tp", pairs) for held in pieces]
        step //= 2
    return pieces


def expert_kernel(count, tile, wide, rows_in, *refs):
    weights_in = refs[: 3 * count]
    out_ref, rows, gates, ups, downs, hidden, row_sem, sems = refs[3 * count :]
    load_rows = pltpu.make_async_copy(rows_in, rows, row_sem)
    load_rows.start()
    loads = []
    for kind, held in enumerate((gates, ups, downs)):
        for j in range(count):
            loads.append(
                pltpu.make_async_copy(
                    weights_in[kind * count + j], held.at[j], sems.at[kind * count + j]
                )
            )
    for j in range(count):
        loads[j].start()
        loads[count + j].start()
    for j in range(count):
        loads[2 * count + j].start()
    load_rows.wait()
    length, width = rows.shape
    for j in range(count):
        loads[j].wait()
        loads[count + j].wait()

        @pl.loop(0, length // tile)
        def _(m):
            here = pl.ds(pl.multiple_of(m * tile, tile), tile)
            block = rows[here, :]
            first = jnp.dot(block, gates[j], preferred_element_type=jnp.float32)
            second = jnp.dot(block, ups[j], preferred_element_type=jnp.float32)
            hidden[j, here, :] = (first / (1.0 + jnp.exp(-first)) * second).astype(jnp.bfloat16)

    for j in range(count):
        loads[2 * count + j].wait()

    @pl.loop(0, width // wide)
    def _(n):
        columns = pl.ds(pl.multiple_of(n * wide, wide), wide)
        for m in range(length // tile):
            here = pl.ds(m * tile, tile)
            total = jnp.dot(
                hidden[0, here, :], downs[0, :, columns], preferred_element_type=jnp.float32
            )
            for j in range(1, count):
                total = total + jnp.dot(
                    hidden[j, here, :], downs[j, :, columns], preferred_element_type=jnp.float32
                )
            out_ref[here, columns] = total.astype(jnp.bfloat16)


def expert_block_local(rows, gates, ups, downs):
    count = len(gates)
    length, width = rows.shape
    part = gates[0].shape[1]
    tile = length // 2
    flops = 6 * length * width * part * count
    anywhere = pl.BlockSpec(memory_space=pl.ANY)
    return pl.pallas_call(
        functools.partial(expert_kernel, count, tile, 256),
        out_shape=jax.ShapeDtypeStruct((length, width), jnp.bfloat16),
        in_specs=[anywhere] * (1 + 3 * count),
        out_specs=pl.BlockSpec(memory_space=pltpu.VMEM),
        scratch_shapes=[
            pltpu.VMEM((length, width), jnp.bfloat16),
            pltpu.VMEM((count, width, part), jnp.bfloat16),
            pltpu.VMEM((count, width, part), jnp.bfloat16),
            pltpu.VMEM((count, part, width), jnp.bfloat16),
            pltpu.VMEM((count, length, part), jnp.bfloat16),
            pltpu.SemaphoreType.DMA(()),
            pltpu.SemaphoreType.DMA((3 * count,)),
        ],
        compiler_params=pltpu.CompilerParams(vmem_limit_bytes=60 * 1024 * 1024),
        cost_estimate=pl.CostEstimate(
            flops=flops,
            bytes_accessed=2 * (2 * length * width + 3 * width * part * count),
            transcendentals=length * part * count,
        ),
    )(rows, *gates, *ups, *downs)


def solution(mesh):
    in_specs = (
        P("ep", None),
        P(),
        P(None, "tp"),
        P(None, "tp"),
        P(None, "tp"),
        P(None, "tp"),
        P("tp", None),
        P(("ep", "tp"), None),
        P(),
        P(("ep", "tp"), None),
        P(("ep", "tp"), None),
        P(("ep", "tp"), None),
        P("ep", None, "tp"),
        P("ep", None, "tp"),
        P("ep", "tp", None),
    )
    out_specs = (P(("ep", "tp"), None), P(("ep", "tp"), None))
    return jax.shard_map(
        on_device, mesh=mesh, in_specs=in_specs, out_specs=out_specs, check_vma=False
    )
```
